32 devices in a mesh: grp: 2 (over x), row: 4 (over z), col: 4 (over y, core).
Axes of the slice: x: 2, y: 2, z: 4, core: 2. Of those that a mesh axis runs over, the one named last changes fastest.
Arguments:
- tokens: bfloat16 [2, 2048, 2048], P('grp', ('row', 'col')), parts along dimension 0, may hold values from -6 to 6
- norm_gain: bfloat16 [2048], replicated, may hold values from 0.099609375 to 1.8984375
- w_in: bfloat16 [2048, 512], replicated, may hold values from -0.125 to 0.125
- w_out: bfloat16 [512, 2048], replicated, may hold values from -0.25 to 0.25
Outputs:
- mixed: bfloat16 [2, 2048, 2048], P('grp', ('row', 'col')), parts along dimension 0
The draws below stay inside these ranges and needn't reach their ends.
There are 2 independent parts, one for each index of `grp`. The reference program is written for one: setup_inputs(seed, part) draws one part's arguments, and reference() takes and returns one part's arrays. A program takes and returns all parts, laid end to end along the dimension named above; an argument that names none is the same for every part. Nothing has to cross between parts.
All inputs are finite; a program needn't handle non-finite values.
Results may differ from the reference program's by a relative error of at most 0.013.
Values may be sent and summed in bfloat16 or wider, within the bound.
A program may use at most 64 MiB of HBM per device.

```python
import jax
import jax.numpy as jnp
from jax import lax

D = 2048
FEATS = 512
GROUP_CH = 128
SEQS = 1
LENGTH = 2048


def level_of(rng, dims, pieces, low, high):
    factor_of = 1.0
    for dim, shards_of in pieces:
        steps = jax.random.uniform(jax.random.fold_in(jax.random.fold_in(rng, 6), dim), (shards_of,), jnp.float32, low / len(pieces), high / len(pieces))
        factor_of = factor_of * jnp.repeat(jnp.exp(steps), dims[dim] // shards_of).reshape((-1,) + (1,) * (len(dims) - 1 - dim))
    return factor_of


def bell_draw(key, shape, spread, bound, split=(), held_as=jnp.bfloat16):
    factor_of = level_of(key, shape, split, -0.22, 0.18) if split else 1.0
    result = jax.random.normal(key, shape, jnp.float32) * spread * factor_of
    return jnp.minimum(jnp.maximum(result, -bound), bound).astype(held_as)


def setup_inputs(seed: int = 0, part: int = 0) -> dict:
    key_of = jax.random.split(jax.random.key(seed), 5)
    part_splits = jax.random.split(jax.random.fold_in(key_of[4], part), 5)
    tokens = bell_draw(part_splits[0], (SEQS, LENGTH, D), 1.0, 6.0, ((1, 16),))
    norm_gain = jnp.clip(1.0 + 0.18 * jax.random.normal(key_of[1], (D,), jnp.float32), 0.099609375, 1.8984375).astype(jnp.bfloat16)
    w_in = bell_draw(key_of[2], (D, FEATS), D ** -0.5, 0.125)
    w_out = bell_draw(key_of[3], (FEATS, D), FEATS ** -0.5, 0.25)
    return {"tokens": tokens, "norm_gain": norm_gain, "w_in": w_in, "w_out": w_out}


def reference(tokens, norm_gain, w_in, w_out):
    widened = tokens.astype(jnp.float32)
    factor = lax.rsqrt(lax.optimization_barrier(jnp.mean(widened * widened, -1, keepdims=True)) + 1e-06)
    normed = (widened * factor * norm_gain.astype(jnp.float32)).astype(jnp.bfloat16)
    flat = normed.reshape(SEQS * LENGTH, D)
    mixin = jnp.dot(flat, w_in, preferred_element_type=jnp.float32).astype(jnp.bfloat16)
    grouped = mixin.astype(jnp.float32).reshape(SEQS, LENGTH, FEATS // GROUP_CH, GROUP_CH)
    spectrum = jnp.fft.fft2(grouped, axes=(1, 3), norm='ortho').real
    spectrum = spectrum.astype(jnp.float32).reshape(SEQS * LENGTH, FEATS).astype(jnp.bfloat16)
    mixed = jnp.dot(spectrum, w_out, preferred_element_type=jnp.float32).astype(jnp.bfloat16)
    return mixed.reshape(SEQS, LENGTH, D)
```

```python
import functools
import math

import jax
import jax.numpy as jnp
import numpy as np
from jax import lax
from jax.experimental import pallas as pl
from jax.experimental.pallas import tpu as pltpu
from jax.sharding import PartitionSpec as P

GROUP_CH = 128


TWO_PI = 2.0 * math.pi
NORM_EPS = 1e-06
HIGHEST = lax.Precision.HIGHEST


def phase_tables(rows, cols, period):
    left = lax.broadcasted_iota(jnp.int32, (rows, cols), 0)
    right = lax.broadcasted_iota(jnp.int32, (rows, cols), 1)
    angles = (left * right % period).astype(jnp.float32) * (TWO_PI / period)
    return (jnp.cos(angles), jnp.sin(angles))


def rotate_by(pattern, cos_table, sin_table, real_part, imag_part):

    def apply(table, data):
        return jnp.einsum(pattern, table, data, precision=HIGHEST)

    return (
        apply(cos_table, real_part) + apply(sin_table, imag_part),
        apply(cos_table, imag_part) - apply(sin_table, real_part),
    )


def twist(real_part, imag_part, cos_table, sin_table):
    return (
        real_part * cos_table + imag_part * sin_table,
        imag_part * cos_table - real_part * sin_table,
    )


def factored_shards(tokens, norm_gain, w_in, w_out):
    seq_count, tok_count, width = tokens.shape
    feat_count = w_in.shape[1]
    row_count = lax.axis_size("row")
    col_count = lax.axis_size("col")
    block_len = tok_count * col_count
    length = block_len * row_count
    sub_feats = feat_count // row_count
    fine_count = tok_count // row_count
    item_count = seq_count * feat_count // col_count
    ortho_scale = 1.0 / math.sqrt(length * GROUP_CH)
    widened = tokens.astype(jnp.float32)
    factor = lax.rsqrt(jnp.mean(widened * widened, -1, keepdims=True) + NORM_EPS)
    normed = (widened * factor * norm_gain.astype(jnp.float32)).astype(jnp.bfloat16)
    mixin = jnp.einsum("std,df->sft", normed, w_in, preferred_element_type=jnp.float32).astype(
        jnp.bfloat16
    )
    row_cos, row_sin = phase_tables(row_count, row_count, row_count)
    chan_cos, chan_sin = phase_tables(GROUP_CH, GROUP_CH, GROUP_CH)
    stacked_shape = (seq_count, sub_feats, row_count, tok_count)
    grouped = mixin.astype(jnp.float32).reshape(
        seq_count, feat_count // GROUP_CH, GROUP_CH, tok_count
    )
    spec_real = jnp.einsum("sgqt,qm->sgmt", grouped, chan_cos, precision=HIGHEST).reshape(
        seq_count, feat_count, tok_count
    )
    spec_imag = -jnp.einsum("sgqt,qm->sgmt", grouped, chan_sin, precision=HIGHEST).reshape(
        seq_count, feat_count, tok_count
    )
    arrived = (
        lax.all_to_all(
            spec_real.astype(jnp.bfloat16), "row", split_axis=1, concat_axis=2, tiled=True
        ).astype(spec_real.dtype),
        lax.all_to_all(
            spec_imag.astype(jnp.bfloat16), "row", split_axis=1, concat_axis=2, tiled=True
        ).astype(spec_imag.dtype),
    )
    stacked_real = arrived[0].reshape(stacked_shape)
    stacked_imag = arrived[1].reshape(stacked_shape)
    real_part, imag_part = rotate_by("ka,sfat->skft", row_cos, row_sin, stacked_real, stacked_imag)
    freq_low = lax.broadcasted_iota(jnp.int32, (row_count, tok_count), 0)
    place = lax.axis_index("col") * tok_count + lax.broadcasted_iota(
        jnp.int32, (row_count, tok_count), 1
    )
    angles = (freq_low * place % length).astype(jnp.float32) * (TWO_PI / length)
    real_part, imag_part = twist(
        real_part, imag_part, jnp.cos(angles)[None, :, None, :], jnp.sin(angles)[None, :, None, :]
    )
    sending = (
        real_part.reshape(item_count, col_count, 1, tok_count),
        imag_part.reshape(item_count, col_count, 1, tok_count),
    )
    col_cos, col_sin = phase_tables(col_count, col_count, col_count)
    mid_cos, mid_sin = phase_tables(col_count, tok_count, block_len)
    tok_cos, tok_sin = phase_tables(tok_count, tok_count, tok_count)
    tok_cos = tok_cos.reshape(row_count, fine_count, tok_count)
    tok_sin = tok_sin.reshape(row_count, fine_count, tok_count)
    span_real, span_imag = rotate_by(
        "uc,qct->qut",
        col_cos,
        col_sin,
        lax.all_to_all(
            sending[0].astype(jnp.bfloat16), "col", split_axis=1, concat_axis=2, tiled=True
        ).astype(jnp.float32)[:, 0],
        lax.all_to_all(
            sending[1].astype(jnp.bfloat16), "col", split_axis=1, concat_axis=2, tiled=True
        ).astype(jnp.float32)[:, 0],
    )
    span_real, span_imag = twist(span_real, span_imag, mid_cos, mid_sin)
    span_real, span_imag = rotate_by("rjt,qut->rjuq", tok_cos, tok_sin, span_real, span_imag)
    owner_shape = (row_count, col_count, fine_count, span_real.shape[-1], 1)
    span_real, span_imag = (span_real.reshape(owner_shape), span_imag.reshape(owner_shape))
    rounded = (span_real * ortho_scale).astype(jnp.bfloat16)
    returned = lax.all_to_all(rounded, "col", split_axis=1, concat_axis=4, tiled=True)
    layout = (row_count, fine_count, seq_count, row_count, sub_feats)
    spectrum = lax.all_to_all(
        returned.reshape(layout), "row", split_axis=0, concat_axis=4, tiled=True
    )
    spectrum = spectrum.reshape(fine_count, seq_count, row_count, feat_count)
    mixed = jnp.einsum("jskf,fd->sjkd", spectrum, w_out, preferred_element_type=jnp.float32).astype(
        jnp.bfloat16
    )
    return mixed.reshape(seq_count, fine_count * row_count, width)


LANES = 128
SUBLANES = 8
MESH = pl.DeviceIdType.MESH
NT = (((1,), (1,)), ((), ()))


def fused_fits(peers, tok_count, feat_count):
    if feat_count % peers or tok_count % peers or GROUP_CH != LANES:
        return False
    slots = feat_count // peers
    return (
        tok_count == LANES
        and slots % (4 * SUBLANES) == 0
        and LANES % slots == 0
        and peers % (LANES // slots) == 0
        and feat_count % GROUP_CH == 0
        and (tok_count // peers) % SUBLANES == 0
    )


def host_tables(peers, tok_count, feat_count):
    length = peers * tok_count
    slots = feat_count // peers
    half = slots // 2
    per_lane = LANES // slots
    stacks = peers // per_lane
    fine = tok_count // peers
    members = GROUP_CH // slots
    chan = np.zeros((GROUP_CH, GROUP_CH))
    chan_at = np.zeros((GROUP_CH,), np.int64)
    q = np.arange(GROUP_CH)
    for m in range(GROUP_CH // 2):
        row = m // half * slots + m % half
        chan[row] = np.cos(2 * np.pi * (q * m % GROUP_CH) / GROUP_CH)
        chan_at[row] = m
        if m:
            chan[row + half] = -np.sin(2 * np.pi * (q * m % GROUP_CH) / GROUP_CH)
            chan_at[row + half] = GROUP_CH - m
        else:
            chan[row + half] = np.cos(np.pi * q)
            chan_at[row + half] = GROUP_CH // 2
    t = np.arange(tok_count)
    b = np.arange(tok_count)[:, None]
    scale = 1.0 / math.sqrt(length * GROUP_CH)
    mid = np.zeros((stacks, tok_count, per_lane, 2, tok_count))
    for g in range(stacks):
        for a in range(per_lane):
            k = peers * b + g * per_lane + a
            angle = 2 * np.pi * (t * k % length) / length
            mid[g, :, a, 0] = np.cos(angle) * scale
            mid[g, :, a, 1] = np.sin(angle) * scale
    mid = mid.reshape(stacks, tok_count, per_lane * 2 * tok_count)
    pick = np.zeros((members, per_lane, slots, per_lane, GROUP_CH))
    for dd in range(members):
        for a in range(per_lane):
            for c in range(slots):
                pick[dd, a, c, a, chan_at[dd * slots + c]] = 1
    pick = pick.reshape(members * LANES, per_lane * GROUP_CH)
    order = np.zeros((tok_count, tok_count))
    for a in range(per_lane):
        for g in range(stacks):
            for f in range(fine):
                order[f * peers + g * per_lane + a, (a * stacks + g) * fine + f] = 1
    return [jnp.asarray(x, jnp.bfloat16) for x in (chan, mid, pick, order)]


def short_transform(blocks):
    n = len(blocks)
    even = [blocks[0]] + [blocks[s] + blocks[n - s] for s in range(1, n // 2)] + [blocks[n // 2]]
    odd = [None] + [blocks[s] - blocks[n - s] for s in range(1, n // 2)]

    def combine(terms):
        groups = {}
        for coef, term in terms:
            if abs(coef) < 1e-9:
                continue
            size = round(abs(coef), 9)
            signed = groups.get(size)
            if signed is None:
                groups[size] = term if coef > 0 else -term
            else:
                groups[size] = signed + term if coef > 0 else signed - term
        total = None
        for size, value in groups.items():
            value = value if size == 1.0 else value * size
            total = value if total is None else total + value
        return total

    out = []
    for a in range(n // 2 + 1):
        cos_part = combine(
            [(math.cos(TWO_PI * (s * a % n) / n), even[s]) for s in range(n // 2 + 1)]
        )
        sin_part = combine([(math.sin(TWO_PI * (s * a % n) / n), odd[s]) for s in range(1, n // 2)])
        if sin_part is None:
            sin_part = jnp.zeros_like(cos_part)
        out.append((cos_part, sin_part))
    for a in range(n // 2 + 1, n):
        out.append((out[n - a][0], -out[n - a][1]))
    return out


def fused_kernel(
    shape,
    tokens_hbm,
    gain_hbm,
    w_in_hbm,
    w_out_hbm,
    chan_hbm,
    mid_hbm,
    pick_hbm,
    order_hbm,
    out_ref,
    tokens,
    gain,
    w_in,
    w_out,
    chan,
    mid,
    pick,
    order,
    first_out,
    first_in,
    blocks,
    second_out,
    second_in,
    load_sem,
    send_a,
    recv_a,
    send_b,
    recv_b,
):
    row_count, col_count = shape
    peers = row_count * col_count
    tok_count, width = tokens.shape
    feat_count = w_in.shape[1]
    slots = feat_count // peers
    half = slots // 2
    per_lane = LANES // slots
    stacks = peers // per_lane
    fine = tok_count // peers
    members = GROUP_CH // slots
    groups = feat_count // GROUP_CH
    me = lax.axis_index("row") * col_count + lax.axis_index("col")

    def peer(step):
        return lax.rem(me + step, peers)

    def device(index):
        return {"row": index // col_count, "col": lax.rem(index, col_count)}

    chunks = 4
    depth = width // chunks
    loads = [
        pltpu.make_async_copy(tokens_hbm, tokens, load_sem.at[0]),
        pltpu.make_async_copy(gain_hbm, gain, load_sem.at[1]),
    ]
    for i in range(chunks):
        part = pl.ds(i * depth, depth)
        loads.append(pltpu.make_async_copy(w_in_hbm.at[part], w_in.at[part], load_sem.at[2 + i]))
    rest = [(chan_hbm, chan), (mid_hbm, mid), (w_out_hbm, w_out), (pick_hbm, pick), (order_hbm, order)]
    for i, (src, dst) in enumerate(rest):
        loads.append(pltpu.make_async_copy(src, dst, load_sem.at[2 + chunks + i]))
    for load in loads:
        load.start()

    barrier = pltpu.get_barrier_semaphore()
    for step in range(1, peers):
        pl.semaphore_signal(barrier, inc=1, device_id=device(peer(step)), device_id_type=MESH)

    loads[0].wait()
    loads[1].wait()
    widened = tokens[...].astype(jnp.float32)
    factor = lax.rsqrt(jnp.mean(widened * widened, -1, keepdims=True) + NORM_EPS)
    normed = (widened * factor * gain[...].astype(jnp.float32)).astype(jnp.bfloat16)
    mixin = None
    for i in range(chunks):
        loads[2 + i].wait()
        term = jnp.dot(
            normed[:, i * depth : (i + 1) * depth],
            w_in[i * depth : (i + 1) * depth, :],
            preferred_element_type=jnp.float32,
        )
        mixin = term if mixin is None else mixin + term
    mixin = mixin.astype(jnp.bfloat16)
    loads[2 + chunks].wait()
    for g in range(groups):
        spec = lax.dot_general(
            chan[...],
            mixin[:, g * GROUP_CH : (g + 1) * GROUP_CH],
            NT,
            preferred_element_type=jnp.float32,
        ).astype(jnp.bfloat16)
        for dd in range(members):
            first_out[g * members + dd] = spec[dd * slots : (dd + 1) * slots]
    pl.semaphore_wait(barrier, peers - 1)
    copies = []
    for step in range(1, peers):
        target = peer(step)
        copy = pltpu.make_async_remote_copy(
            src_ref=first_out.at[target],
            dst_ref=first_in.at[me],
            send_sem=send_a.at[step],
            recv_sem=recv_a.at[step],
            device_id=device(target),
            device_id_type=MESH,
        )
        copy.start()
        copies.append(copy)
    first_in[me] = first_out[me]
    blocks[...] = jnp.zeros_like(blocks)
    for load in loads[3 + chunks :]:
        load.wait()
    for copy in copies:
        copy.wait_recv()

    arrived = [first_in[s].astype(jnp.float32) for s in range(peers)]
    place = lax.broadcasted_iota(jnp.int32, (half, tok_count), 0) + me * half
    paired = lax.rem(place, GROUP_CH // 2) != 0
    spectra = short_transform(arrived)
    for a, (cos_part, sin_part) in enumerate(spectra):
        a_cos, b_cos = cos_part[:half], cos_part[half:]
        a_sin, b_sin = sin_part[:half], sin_part[half:]
        top_cos = jnp.where(paired, a_cos + b_sin, a_cos)
        top_sin = jnp.where(paired, b_cos - a_sin, -a_sin)
        low_cos = jnp.where(paired, a_cos - b_sin, b_cos)
        low_sin = jnp.where(paired, -a_sin - b_cos, -b_sin)
        at = a % per_lane
        left = at * 2 * tok_count
        blocks[a // per_lane, at * slots : at * slots + half, left : left + tok_count] = (
            top_cos.astype(jnp.bfloat16)
        )
        blocks[
            a // per_lane, at * slots : at * slots + half, left + tok_count : left + 2 * tok_count
        ] = top_sin.astype(jnp.bfloat16)
        blocks[a // per_lane, at * slots + half : (at + 1) * slots, left : left + tok_count] = (
            low_cos.astype(jnp.bfloat16)
        )
        blocks[
            a // per_lane,
            at * slots + half : (at + 1) * slots,
            left + tok_count : left + 2 * tok_count,
        ] = low_sin.astype(jnp.bfloat16)
    found = []
    for g in range(stacks):
        value = lax.dot_general(mid[g], blocks[g], NT, preferred_element_type=jnp.float32)
        found.append(value.reshape(peers, fine, LANES))
    second_out[...] = jnp.concatenate(found, axis=1).astype(jnp.bfloat16)

    def landing(index):
        lanes = pl.ds(pl.multiple_of(lax.rem(index, members) * LANES, LANES), LANES)
        return second_in.at[index // members, :, lanes]

    returns = []
    for step in range(1, peers):
        target = peer(step)
        copy = pltpu.make_async_remote_copy(
            src_ref=second_out.at[target],
            dst_ref=landing(me),
            send_sem=send_b.at[step],
            recv_sem=recv_b.at[step],
            device_id=device(target),
            device_id_type=MESH,
        )
        copy.start()
        returns.append(copy)
    landing(me)[...] = second_out[me]
    for copy in copies:
        copy.wait_send()
    for copy in returns:
        copy.wait_recv()
    flat = second_in[...].reshape(groups * stacks * fine, members * LANES)
    picked = jnp.dot(flat, pick[...], preferred_element_type=jnp.float32).astype(jnp.bfloat16)
    rows = stacks * fine
    gathered = jnp.concatenate(
        [
            jnp.concatenate(
                [
                    picked[g * rows : (g + 1) * rows, a * GROUP_CH : (a + 1) * GROUP_CH]
                    for g in range(groups)
                ],
                axis=1,
            )
            for a in range(per_lane)
        ],
        axis=0,
    )
    spectrum = jnp.dot(order[...], gathered, preferred_element_type=jnp.float32).astype(
        jnp.bfloat16
    )
    out_ref[...] = jnp.dot(spectrum, w_out[...], preferred_element_type=jnp.float32).astype(
        out_ref.dtype
    )
    for copy in returns:
        copy.wait_send()


def fused_shards(tokens, norm_gain, w_in, w_out):
    seq_count, tok_count, width = tokens.shape
    feat_count = w_in.shape[1]
    shape = (lax.axis_size("row"), lax.axis_size("col"))
    peers = shape[0] * shape[1]
    slots = feat_count // peers
    per_lane = LANES // slots
    stacks = peers // per_lane
    fine = tok_count // peers
    members = GROUP_CH // slots
    tables = host_tables(peers, tok_count, feat_count)
    operands = [tokens.reshape(tok_count, width), norm_gain.reshape(1, width), w_in, w_out, *tables]
    held = [pltpu.VMEM(x.shape, x.dtype) for x in operands]
    mixed = pl.pallas_call(
        functools.partial(fused_kernel, shape),
        out_shape=jax.ShapeDtypeStruct((tok_count, width), jnp.bfloat16),
        in_specs=[pl.BlockSpec(memory_space=pl.ANY)] * len(operands),
        out_specs=pl.BlockSpec(memory_space=pltpu.VMEM),
        scratch_shapes=held
        + [
            pltpu.VMEM((peers, slots, tok_count), jnp.bfloat16),
            pltpu.VMEM((peers, slots, tok_count), jnp.bfloat16),
            pltpu.VMEM((stacks, LANES, per_lane * 2 * tok_count), jnp.bfloat16),
            pltpu.VMEM((peers, stacks * fine, LANES), jnp.bfloat16),
            pltpu.VMEM((peers // members, stacks * fine, members * LANES), jnp.bfloat16),
            pltpu.SemaphoreType.DMA((16,)),
            pltpu.SemaphoreType.DMA((peers,)),
            pltpu.SemaphoreType.DMA((peers,)),
            pltpu.SemaphoreType.DMA((peers,)),
            pltpu.SemaphoreType.DMA((peers,)),
        ],
        compiler_params=pltpu.CompilerParams(collective_id=0, has_side_effects=True),
    )(*operands)
    return mixed.reshape(seq_count, tok_count, width)


def shards(tokens, norm_gain, w_in, w_out):
    peers = lax.axis_size("row") * lax.axis_size("col")
    seq_count, tok_count, _ = tokens.shape
    if seq_count == 1 and fused_fits(peers, tok_count, w_in.shape[1]):
        return fused_shards(tokens, norm_gain, w_in, w_out)
    return factored_shards(tokens, norm_gain, w_in, w_out)


def solution(mesh):
    return jax.shard_map(
        shards,
        mesh=mesh,
        in_specs=(P("grp", ("row", "col"), None), P(), P(), P()),
        out_specs=P("grp", ("row", "col"), None),
        check_vma=False,
    )
```

```python
import functools
import math

import jax
import jax.numpy as jnp
import numpy as np
from jax import lax
from jax.experimental import pallas as pl
from jax.experimental.pallas import tpu as pltpu
from jax.sharding import PartitionSpec as P

GROUP_CH = 128


TWO_PI = 2.0 * math.pi
NORM_EPS = 1e-06
HIGHEST = lax.Precision.HIGHEST


def phase_tables(rows, cols, period):
    left = lax.broadcasted_iota(jnp.int32, (rows, cols), 0)
    right = lax.broadcasted_iota(jnp.int32, (rows, cols), 1)
    angles = (left * right % period).astype(jnp.float32) * (TWO_PI / period)
    return (jnp.cos(angles), jnp.sin(angles))


def rotate_by(pattern, cos_table, sin_table, real_part, imag_part):

    def apply(table, data):
        return jnp.einsum(pattern, table, data, precision=HIGHEST)

    return (
        apply(cos_table, real_part) + apply(sin_table, imag_part),
        apply(cos_table, imag_part) - apply(sin_table, real_part),
    )


def twist(real_part, imag_part, cos_table, sin_table):
    return (
        real_part * cos_table + imag_part * sin_table,
        imag_part * cos_table - real_part * sin_table,
    )


def factored_shards(tokens, norm_gain, w_in, w_out):
    seq_count, tok_count, width = tokens.shape
    feat_count = w_in.shape[1]
    row_count = lax.axis_size("row")
    col_count = lax.axis_size("col")
    block_len = tok_count * col_count
    length = block_len * row_count
    sub_feats = feat_count // row_count
    fine_count = tok_count // row_count
    item_count = seq_count * feat_count // col_count
    ortho_scale = 1.0 / math.sqrt(length * GROUP_CH)
    widened = tokens.astype(jnp.float32)
    factor = lax.rsqrt(jnp.mean(widened * widened, -1, keepdims=True) + NORM_EPS)
    normed = (widened * factor * norm_gain.astype(jnp.float32)).astype(jnp.bfloat16)
    mixin = jnp.einsum("std,df->sft", normed, w_in, preferred_element_type=jnp.float32).astype(
        jnp.bfloat16
    )
    row_cos, row_sin = phase_tables(row_count, row_count, row_count)
    chan_cos, chan_sin = phase_tables(GROUP_CH, GROUP_CH, GROUP_CH)
    stacked_shape = (seq_count, sub_feats, row_count, tok_count)
    grouped = mixin.astype(jnp.float32).reshape(
        seq_count, feat_count // GROUP_CH, GROUP_CH, tok_count
    )
    spec_real = jnp.einsum("sgqt,qm->sgmt", grouped, chan_cos, precision=HIGHEST).reshape(
        seq_count, feat_count, tok_count
    )
    spec_imag = -jnp.einsum("sgqt,qm->sgmt", grouped, chan_sin, precision=HIGHEST).reshape(
        seq_count, feat_count, tok_count
    )
    arrived = (
        lax.all_to_all(
            spec_real.astype(jnp.bfloat16), "row", split_axis=1, concat_axis=2, tiled=True
        ).astype(spec_real.dtype),
        lax.all_to_all(
            spec_imag.astype(jnp.bfloat16), "row", split_axis=1, concat_axis=2, tiled=True
        ).astype(spec_imag.dtype),
    )
    stacked_real = arrived[0].reshape(stacked_shape)
    stacked_imag = arrived[1].reshape(stacked_shape)
    real_part, imag_part = rotate_by("ka,sfat->skft", row_cos, row_sin, stacked_real, stacked_imag)
    freq_low = lax.broadcasted_iota(jnp.int32, (row_count, tok_count), 0)
    place = lax.axis_index("col") * tok_count + lax.broadcasted_iota(
        jnp.int32, (row_count, tok_count), 1
    )
    angles = (freq_low * place % length).astype(jnp.float32) * (TWO_PI / length)
    real_part, imag_part = twist(
        real_part, imag_part, jnp.cos(angles)[None, :, None, :], jnp.sin(angles)[None, :, None, :]
    )
    sending = (
        real_part.reshape(item_count, col_count, 1, tok_count),
        imag_part.reshape(item_count, col_count, 1, tok_count),
    )
    col_cos, col_sin = phase_tables(col_count, col_count, col_count)
    mid_cos, mid_sin = phase_tables(col_count, tok_count, block_len)
    tok_cos, tok_sin = phase_tables(tok_count, tok_count, tok_count)
    tok_cos = tok_cos.reshape(row_count, fine_count, tok_count)
    tok_sin = tok_sin.reshape(row_count, fine_count, tok_count)
    span_real, span_imag = rotate_by(
        "uc,qct->qut",
        col_cos,
        col_sin,
        lax.all_to_all(
            sending[0].astype(jnp.bfloat16), "col", split_axis=1, concat_axis=2, tiled=True
        ).astype(jnp.float32)[:, 0],
        lax.all_to_all(
            sending[1].astype(jnp.bfloat16), "col", split_axis=1, concat_axis=2, tiled=True
        ).astype(jnp.float32)[:, 0],
    )
    span_real, span_imag = twist(span_real, span_imag, mid_cos, mid_sin)
    span_real, span_imag = rotate_by("rjt,qut->rjuq", tok_cos, tok_sin, span_real, span_imag)
    owner_shape = (row_count, col_count, fine_count, span_real.shape[-1], 1)
    span_real, span_imag = (span_real.reshape(owner_shape), span_imag.reshape(owner_shape))
    rounded = (span_real * ortho_scale).astype(jnp.bfloat16)
    returned = lax.all_to_all(rounded, "col", split_axis=1, concat_axis=4, tiled=True)
    layout = (row_count, fine_count, seq_count, row_count, sub_feats)
    spectrum = lax.all_to_all(
        returned.reshape(layout), "row", split_axis=0, concat_axis=4, tiled=True
    )
    spectrum = spectrum.reshape(fine_count, seq_count, row_count, feat_count)
    mixed = jnp.einsum("jskf,fd->sjkd", spectrum, w_out, preferred_element_type=jnp.float32).astype(
        jnp.bfloat16
    )
    return mixed.reshape(seq_count, fine_count * row_count, width)


LANES = 128
SUBLANES = 8
MESH = pl.DeviceIdType.MESH
NT = (((1,), (1,)), ((), ()))


def fused_fits(peers, tok_count, feat_count):
    if feat_count % peers or tok_count % peers or GROUP_CH != LANES:
        return False
    slots = feat_count // peers
    return (
        tok_count == LANES
        and slots % (4 * SUBLANES) == 0
        and LANES % slots == 0
        and peers % (LANES // slots) == 0
        and feat_count % GROUP_CH == 0
        and (tok_count // peers) % SUBLANES == 0
    )


def host_tables(peers, tok_count, feat_count):
    length = peers * tok_count
    slots = feat_count // peers
    half = slots // 2
    per_lane = LANES // slots
    stacks = peers // per_lane
    fine = tok_count // peers
    members = GROUP_CH // slots
    chan = np.zeros((GROUP_CH, GROUP_CH))
    chan_at = np.zeros((GROUP_CH,), np.int64)
    q = np.arange(GROUP_CH)
    for m in range(GROUP_CH // 2):
        row = m // half * slots + m % half
        chan[row] = np.cos(2 * np.pi * (q * m % GROUP_CH) / GROUP_CH)
        chan_at[row] = m
        if m:
            chan[row + half] = -np.sin(2 * np.pi * (q * m % GROUP_CH) / GROUP_CH)
            chan_at[row + half] = GROUP_CH - m
        else:
            chan[row + half] = np.cos(np.pi * q)
            chan_at[row + half] = GROUP_CH // 2
    t = np.arange(tok_count)
    b = np.arange(tok_count)[:, None]
    scale = 1.0 / math.sqrt(length * GROUP_CH)
    mid = np.zeros((stacks, tok_count, per_lane, 2, tok_count))
    for g in range(stacks):
        for a in range(per_lane):
            k = peers * b + g * per_lane + a
            angle = 2 * np.pi * (t * k % length) / length
            mid[g, :, a, 0] = np.cos(angle) * scale
            mid[g, :, a, 1] = np.sin(angle) * scale
    mid = mid.reshape(stacks, tok_count, per_lane * 2 * tok_count)
    pick = np.zeros((members, per_lane, slots, per_lane, GROUP_CH))
    for dd in range(members):
        for a in range(per_lane):
            for c in range(slots):
                pick[dd, a, c, a, chan_at[dd * slots + c]] = 1
    pick = pick.reshape(members * LANES, per_lane * GROUP_CH)
    return [jnp.asarray(x, jnp.bfloat16) for x in (chan, mid, pick)]


def short_transform(blocks):
    n = len(blocks)
    even = [blocks[0]] + [blocks[s] + blocks[n - s] for s in range(1, n // 2)] + [blocks[n // 2]]
    odd = [None] + [blocks[s] - blocks[n - s] for s in range(1, n // 2)]

    def combine(terms):
        groups = {}
        for coef, term in terms:
            if abs(coef) < 1e-9:
                continue
            size = round(abs(coef), 9)
            signed = groups.get(size)
            if signed is None:
                groups[size] = term if coef > 0 else -term
            else:
                groups[size] = signed + term if coef > 0 else signed - term
        total = None
        for size, value in groups.items():
            value = value if size == 1.0 else value * size
            total = value if total is None else total + value
        return total

    out = []
    for a in range(n // 2 + 1):
        cos_part = combine(
            [(math.cos(TWO_PI * (s * a % n) / n), even[s]) for s in range(n // 2 + 1)]
        )
        sin_part = combine([(math.sin(TWO_PI * (s * a % n) / n), odd[s]) for s in range(1, n // 2)])
        if sin_part is None:
            sin_part = jnp.zeros_like(cos_part)
        out.append((cos_part, sin_part))
    for a in range(n // 2 + 1, n):
        out.append((out[n - a][0], -out[n - a][1]))
    return out


def fused_kernel(
    shape,
    tokens_hbm,
    gain_hbm,
    w_in_hbm,
    chan_hbm,
    mid_hbm,
    pick_hbm,
    out_ref,
    tokens,
    gain,
    w_in,
    chan,
    mid,
    pick,
    natural,
    first_out,
    first_in,
    blocks,
    second_out,
    second_in,
    load_sem,
    send_a,
    recv_a,
    send_b,
    recv_b,
):
    row_count, col_count = shape
    peers = row_count * col_count
    tok_count, width = tokens.shape
    feat_count = w_in.shape[1]
    slots = feat_count // peers
    half = slots // 2
    per_lane = LANES // slots
    stacks = peers // per_lane
    fine = tok_count // peers
    members = GROUP_CH // slots
    groups = feat_count // GROUP_CH
    me = lax.axis_index("row") * col_count + lax.axis_index("col")

    def peer(step):
        return lax.rem(me + step, peers)

    def device(index):
        return {"row": index // col_count, "col": lax.rem(index, col_count)}

    chunks = 4
    depth = width // chunks
    loads = [
        pltpu.make_async_copy(tokens_hbm, tokens, load_sem.at[0]),
        pltpu.make_async_copy(gain_hbm, gain, load_sem.at[1]),
    ]
    for i in range(chunks):
        part = pl.ds(i * depth, depth)
        loads.append(pltpu.make_async_copy(w_in_hbm.at[part], w_in.at[part], load_sem.at[2 + i]))
    rest = [(chan_hbm, chan), (mid_hbm, mid), (pick_hbm, pick)]
    for i, (src, dst) in enumerate(rest):
        loads.append(pltpu.make_async_copy(src, dst, load_sem.at[2 + chunks + i]))
    for load in loads[: 3 + chunks]:
        load.start()

    barrier = pltpu.get_barrier_semaphore()
    for step in range(1, peers):
        pl.semaphore_signal(barrier, inc=1, device_id=device(peer(step)), device_id_type=MESH)

    loads[0].wait()
    loads[1].wait()
    widened = tokens[...].astype(jnp.float32)
    factor = lax.rsqrt(jnp.mean(widened * widened, -1, keepdims=True) + NORM_EPS)
    normed = (widened * factor * gain[...].astype(jnp.float32).reshape(1, width)).astype(jnp.bfloat16)
    mixin = None
    for i in range(chunks):
        loads[2 + i].wait()
        term = jnp.dot(
            normed[:, i * depth : (i + 1) * depth],
            w_in[i * depth : (i + 1) * depth, :],
            preferred_element_type=jnp.float32,
        )
        mixin = term if mixin is None else mixin + term
    mixin = mixin.astype(jnp.bfloat16)
    for load in loads[3 + chunks :]:
        load.start()
    loads[2 + chunks].wait()
    for g in range(groups):
        spec = lax.dot_general(
            chan[...],
            mixin[:, g * GROUP_CH : (g + 1) * GROUP_CH],
            NT,
            preferred_element_type=jnp.float32,
        ).astype(jnp.bfloat16)
        for dd in range(members):
            first_out[g * members + dd] = spec[dd * slots : (dd + 1) * slots]
    pl.semaphore_wait(barrier, peers - 1)
    copies = []
    for step in range(1, peers):
        target = peer(step)
        copy = pltpu.make_async_remote_copy(
            src_ref=first_out.at[target],
            dst_ref=first_in.at[me],
            send_sem=send_a.at[step],
            recv_sem=recv_a.at[step],
            device_id=device(target),
            device_id_type=MESH,
        )
        copy.start()
        copies.append(copy)
    first_in[me] = first_out[me]
    blocks[...] = jnp.zeros_like(blocks)
    for load in loads[3 + chunks :]:
        load.wait()
    for copy in copies:
        copy.wait_recv()

    arrived = [first_in[s].astype(jnp.float32) for s in range(peers)]
    place = lax.broadcasted_iota(jnp.int32, (half, tok_count), 0) + me * half
    paired = lax.rem(place, GROUP_CH // 2) != 0
    spectra = short_transform(arrived)
    for a, (cos_part, sin_part) in enumerate(spectra):
        a_cos, b_cos = cos_part[:half], cos_part[half:]
        a_sin, b_sin = sin_part[:half], sin_part[half:]
        top_cos = jnp.where(paired, a_cos + b_sin, a_cos)
        top_sin = jnp.where(paired, b_cos - a_sin, -a_sin)
        low_cos = jnp.where(paired, a_cos - b_sin, b_cos)
        low_sin = jnp.where(paired, -a_sin - b_cos, -b_sin)
        at = a % per_lane
        left = at * 2 * tok_count
        blocks[a // per_lane, at * slots : at * slots + half, left : left + tok_count] = (
            top_cos.astype(jnp.bfloat16)
        )
        blocks[
            a // per_lane, at * slots : at * slots + half, left + tok_count : left + 2 * tok_count
        ] = top_sin.astype(jnp.bfloat16)
        blocks[a // per_lane, at * slots + half : (at + 1) * slots, left : left + tok_count] = (
            low_cos.astype(jnp.bfloat16)
        )
        blocks[
            a // per_lane,
            at * slots + half : (at + 1) * slots,
            left + tok_count : left + 2 * tok_count,
        ] = low_sin.astype(jnp.bfloat16)
    found = []
    for g in range(stacks):
        value = lax.dot_general(mid[g], blocks[g], NT, preferred_element_type=jnp.float32)
        found.append(value.reshape(peers, fine, LANES))
    second_out[...] = jnp.concatenate(found, axis=1).astype(jnp.bfloat16)

    def landing(index):
        lanes = pl.ds(pl.multiple_of(lax.rem(index, members) * LANES, LANES), LANES)
        return second_in.at[index // members, :, lanes]

    returns = []
    for step in range(1, peers):
        target = peer(step)
        copy = pltpu.make_async_remote_copy(
            src_ref=second_out.at[target],
            dst_ref=landing(me),
            send_sem=send_b.at[step],
            recv_sem=recv_b.at[step],
            device_id=device(target),
            device_id_type=MESH,
        )
        copy.start()
        returns.append(copy)
    landing(me)[...] = second_out[me]
    for copy in copies:
        copy.wait_send()
    for copy in returns:
        copy.wait_recv()
    flat = second_in[...].reshape(groups * stacks * fine, members * LANES)
    picked = jnp.dot(flat, pick[...], preferred_element_type=jnp.float32)
    for group in range(groups):
        for g in range(stacks):
            top = (group * stacks + g) * fine
            for a in range(per_lane):
                natural[group, pl.ds(g * per_lane + a, fine, stride=peers), :] = picked[top : top + fine, a * GROUP_CH : (a + 1) * GROUP_CH]
        out_ref[:, group * GROUP_CH : (group + 1) * GROUP_CH] = natural[group].astype(
            out_ref.dtype
        )
    for copy in returns:
        copy.wait_send()


def project_kernel(chunks, spectrum, w_out, out_hbm, staged, sems):
    size = w_out.shape[1] // chunks
    copies = []
    for i in range(chunks):
        lanes = slice(i * size, (i + 1) * size)
        staged[:, lanes] = jnp.dot(
            spectrum[...], w_out[:, lanes], preferred_element_type=jnp.float32
        ).astype(staged.dtype)
        span = pl.ds(i * size, size)
        copy = pltpu.make_async_copy(staged.at[:, span], out_hbm.at[:, span], sems.at[i])
        copy.start()
        copies.append(copy)
    for copy in copies:
        copy.wait()


def fused_shards(tokens, norm_gain, w_in, w_out):
    seq_count, tok_count, width = tokens.shape
    feat_count = w_in.shape[1]
    shape = (lax.axis_size("row"), lax.axis_size("col"))
    peers = shape[0] * shape[1]
    slots = feat_count // peers
    per_lane = LANES // slots
    stacks = peers // per_lane
    fine = tok_count // peers
    members = GROUP_CH // slots
    tables = host_tables(peers, tok_count, feat_count)
    operands = [tokens.reshape(tok_count, width), norm_gain, w_in, *tables]
    held = [pltpu.VMEM(x.shape, x.dtype) for x in operands]
    spectrum = pl.pallas_call(
        functools.partial(fused_kernel, shape),
        out_shape=pltpu.VMEM((tok_count, feat_count), jnp.bfloat16),
        in_specs=[pl.BlockSpec(memory_space=pltpu.HBM)] * len(operands),
        out_specs=pl.BlockSpec(memory_space=pltpu.VMEM),
        scratch_shapes=held
        + [
            pltpu.VMEM((feat_count // GROUP_CH, tok_count, GROUP_CH), jnp.float32),
            pltpu.VMEM((peers, slots, tok_count), jnp.bfloat16),
            pltpu.VMEM((peers, slots, tok_count), jnp.bfloat16),
            pltpu.VMEM((stacks, LANES, per_lane * 2 * tok_count), jnp.bfloat16),
            pltpu.VMEM((peers, stacks * fine, LANES), jnp.bfloat16),
            pltpu.VMEM((peers // members, stacks * fine, members * LANES), jnp.bfloat16),
            pltpu.SemaphoreType.DMA((16,)),
            pltpu.SemaphoreType.DMA((peers,)),
            pltpu.SemaphoreType.DMA((peers,)),
            pltpu.SemaphoreType.DMA((peers,)),
            pltpu.SemaphoreType.DMA((peers,)),
        ],
        compiler_params=pltpu.CompilerParams(
            collective_id=0, has_side_effects=True, vmem_limit_bytes=64_600_000
        ),
    )(*operands)
    chunks = max(1, width // 512)
    mixed = pl.pallas_call(
        functools.partial(project_kernel, chunks),
        out_shape=jax.ShapeDtypeStruct((tok_count, width), jnp.bfloat16),
        in_specs=[pl.BlockSpec(memory_space=pltpu.VMEM)] * 2,
        out_specs=pl.BlockSpec(memory_space=pltpu.HBM),
        scratch_shapes=[
            pltpu.VMEM((tok_count, width), jnp.bfloat16),
            pltpu.SemaphoreType.DMA((chunks,)),
        ],
        compiler_params=pltpu.CompilerParams(vmem_limit_bytes=8 * 1024 * 1024),
    )(spectrum, w_out)
    return mixed.reshape(seq_count, tok_count, width)


def shards(tokens, norm_gain, w_in, w_out):
    peers = lax.axis_size("row") * lax.axis_size("col")
    seq_count, tok_count, _ = tokens.shape
    if seq_count == 1 and fused_fits(peers, tok_count, w_in.shape[1]):
        return fused_shards(tokens, norm_gain, w_in, w_out)
    return factored_shards(tokens, norm_gain, w_in, w_out)


def solution(mesh):
    return jax.shard_map(
        shards,
        mesh=mesh,
        in_specs=(P("grp", ("row", "col"), None), P(), P(), P()),
        out_specs=P("grp", ("row", "col"), None),
        check_vma=False,
    )
```

```python
import functools
import math

import jax
import jax.numpy as jnp
import numpy as np
from jax import lax
from jax.experimental import pallas as pl
from jax.experimental.pallas import tpu as pltpu
from jax.sharding import PartitionSpec as P

GROUP_CH = 128


TWO_PI = 2.0 * math.pi
NORM_EPS = 1e-06
HIGHEST = lax.Precision.HIGHEST


def phase_tables(rows, cols, period):
    left = lax.broadcasted_iota(jnp.int32, (rows, cols), 0)
    right = lax.broadcasted_iota(jnp.int32, (rows, cols), 1)
    angles = (left * right % period).astype(jnp.float32) * (TWO_PI / period)
    return (jnp.cos(angles), jnp.sin(angles))


def rotate_by(pattern, cos_table, sin_table, real_part, imag_part):

    def apply(table, data):
        return jnp.einsum(pattern, table, data, precision=HIGHEST)

    return (
        apply(cos_table, real_part) + apply(sin_table, imag_part),
        apply(cos_table, imag_part) - apply(sin_table, real_part),
    )


def twist(real_part, imag_part, cos_table, sin_table):
    return (
        real_part * cos_table + imag_part * sin_table,
        imag_part * cos_table - real_part * sin_table,
    )


def factored_shards(tokens, norm_gain, w_in, w_out):
    seq_count, tok_count, width = tokens.shape
    feat_count = w_in.shape[1]
    row_count = lax.axis_size("row")
    col_count = lax.axis_size("col")
    block_len = tok_count * col_count
    length = block_len * row_count
    sub_feats = feat_count // row_count
    fine_count = tok_count // row_count
    item_count = seq_count * feat_count // col_count
    ortho_scale = 1.0 / math.sqrt(length * GROUP_CH)
    widened = tokens.astype(jnp.float32)
    factor = lax.rsqrt(jnp.mean(widened * widened, -1, keepdims=True) + NORM_EPS)
    normed = (widened * factor * norm_gain.astype(jnp.float32)).astype(jnp.bfloat16)
    mixin = jnp.einsum("std,df->sft", normed, w_in, preferred_element_type=jnp.float32).astype(
        jnp.bfloat16
    )
    row_cos, row_sin = phase_tables(row_count, row_count, row_count)
    chan_cos, chan_sin = phase_tables(GROUP_CH, GROUP_CH, GROUP_CH)
    stacked_shape = (seq_count, sub_feats, row_count, tok_count)
    grouped = mixin.astype(jnp.float32).reshape(
        seq_count, feat_count // GROUP_CH, GROUP_CH, tok_count
    )
    spec_real = jnp.einsum("sgqt,qm->sgmt", grouped, chan_cos, precision=HIGHEST).reshape(
        seq_count, feat_count, tok_count
    )
    spec_imag = -jnp.einsum("sgqt,qm->sgmt", grouped, chan_sin, precision=HIGHEST).reshape(
        seq_count, feat_count, tok_count
    )
    arrived = (
        lax.all_to_all(
            spec_real.astype(jnp.bfloat16), "row", split_axis=1, concat_axis=2, tiled=True
        ).astype(spec_real.dtype),
        lax.all_to_all(
            spec_imag.astype(jnp.bfloat16), "row", split_axis=1, concat_axis=2, tiled=True
        ).astype(spec_imag.dtype),
    )
    stacked_real = arrived[0].reshape(stacked_shape)
    stacked_imag = arrived[1].reshape(stacked_shape)
    real_part, imag_part = rotate_by("ka,sfat->skft", row_cos, row_sin, stacked_real, stacked_imag)
    freq_low = lax.broadcasted_iota(jnp.int32, (row_count, tok_count), 0)
    place = lax.axis_index("col") * tok_count + lax.broadcasted_iota(
        jnp.int32, (row_count, tok_count), 1
    )
    angles = (freq_low * place % length).astype(jnp.float32) * (TWO_PI / length)
    real_part, imag_part = twist(
        real_part, imag_part, jnp.cos(angles)[None, :, None, :], jnp.sin(angles)[None, :, None, :]
    )
    sending = (
        real_part.reshape(item_count, col_count, 1, tok_count),
        imag_part.reshape(item_count, col_count, 1, tok_count),
    )
    col_cos, col_sin = phase_tables(col_count, col_count, col_count)
    mid_cos, mid_sin = phase_tables(col_count, tok_count, block_len)
    tok_cos, tok_sin = phase_tables(tok_count, tok_count, tok_count)
    tok_cos = tok_cos.reshape(row_count, fine_count, tok_count)
    tok_sin = tok_sin.reshape(row_count, fine_count, tok_count)
    span_real, span_imag = rotate_by(
        "uc,qct->qut",
        col_cos,
        col_sin,
        lax.all_to_all(
            sending[0].astype(jnp.bfloat16), "col", split_axis=1, concat_axis=2, tiled=True
        ).astype(jnp.float32)[:, 0],
        lax.all_to_all(
            sending[1].astype(jnp.bfloat16), "col", split_axis=1, concat_axis=2, tiled=True
        ).astype(jnp.float32)[:, 0],
    )
    span_real, span_imag = twist(span_real, span_imag, mid_cos, mid_sin)
    span_real, span_imag = rotate_by("rjt,qut->rjuq", tok_cos, tok_sin, span_real, span_imag)
    owner_shape = (row_count, col_count, fine_count, span_real.shape[-1], 1)
    span_real, span_imag = (span_real.reshape(owner_shape), span_imag.reshape(owner_shape))
    rounded = (span_real * ortho_scale).astype(jnp.bfloat16)
    returned = lax.all_to_all(rounded, "col", split_axis=1, concat_axis=4, tiled=True)
    layout = (row_count, fine_count, seq_count, row_count, sub_feats)
    spectrum = lax.all_to_all(
        returned.reshape(layout), "row", split_axis=0, concat_axis=4, tiled=True
    )
    spectrum = spectrum.reshape(fine_count, seq_count, row_count, feat_count)
    mixed = jnp.einsum("jskf,fd->sjkd", spectrum, w_out, preferred_element_type=jnp.float32).astype(
        jnp.bfloat16
    )
    return mixed.reshape(seq_count, fine_count * row_count, width)


LANES = 128
SUBLANES = 8
MESH = pl.DeviceIdType.MESH
NT = (((1,), (1,)), ((), ()))


def fused_fits(peers, tok_count, feat_count):
    if feat_count % peers or tok_count % peers or GROUP_CH != LANES:
        return False
    slots = feat_count // peers
    return (
        tok_count == LANES
        and slots % (4 * SUBLANES) == 0
        and LANES % slots == 0
        and peers % (LANES // slots) == 0
        and feat_count % GROUP_CH == 0
        and (tok_count // peers) % SUBLANES == 0
    )


def host_tables(peers, tok_count, feat_count):
    length = peers * tok_count
    slots = feat_count // peers
    half = slots // 2
    per_lane = LANES // slots
    stacks = peers // per_lane
    fine = tok_count // peers
    members = GROUP_CH // slots
    chan = np.zeros((GROUP_CH, GROUP_CH))
    chan_at = np.zeros((GROUP_CH,), np.int64)
    q = np.arange(GROUP_CH)
    for m in range(GROUP_CH // 2):
        row = m // half * slots + m % half
        chan[row] = np.cos(2 * np.pi * (q * m % GROUP_CH) / GROUP_CH)
        chan_at[row] = m
        if m:
            chan[row + half] = -np.sin(2 * np.pi * (q * m % GROUP_CH) / GROUP_CH)
            chan_at[row + half] = GROUP_CH - m
        else:
            chan[row + half] = np.cos(np.pi * q)
            chan_at[row + half] = GROUP_CH // 2
    t = np.arange(tok_count)
    b = np.arange(tok_count)[:, None]
    scale = 1.0 / math.sqrt(length * GROUP_CH)
    mid = np.zeros((stacks, tok_count, per_lane, 2, tok_count))
    for g in range(stacks):
        for a in range(per_lane):
            k = peers * b + g * per_lane + a
            angle = 2 * np.pi * (t * k % length) / length
            mid[g, :, a, 0] = np.cos(angle) * scale
            mid[g, :, a, 1] = np.sin(angle) * scale
    mid = mid.reshape(stacks, tok_count, per_lane * 2 * tok_count)
    pick = np.zeros((members, per_lane, slots, per_lane, GROUP_CH))
    for dd in range(members):
        for a in range(per_lane):
            for c in range(slots):
                pick[dd, a, c, a, chan_at[dd * slots + c]] = 1
    pick = pick.reshape(members * LANES, per_lane * GROUP_CH)
    return [jnp.asarray(x, jnp.bfloat16) for x in (chan, mid, pick)]


def short_transform(blocks):
    n = len(blocks)
    even = [blocks[0]] + [blocks[s] + blocks[n - s] for s in range(1, n // 2)] + [blocks[n // 2]]
    odd = [None] + [blocks[s] - blocks[n - s] for s in range(1, n // 2)]

    def combine(terms):
        groups = {}
        for coef, term in terms:
            if abs(coef) < 1e-9:
                continue
            size = round(abs(coef), 9)
            signed = groups.get(size)
            if signed is None:
                groups[size] = term if coef > 0 else -term
            else:
                groups[size] = signed + term if coef > 0 else signed - term
        total = None
        for size, value in groups.items():
            value = value if size == 1.0 else value * size
            total = value if total is None else total + value
        return total

    out = []
    for a in range(n // 2 + 1):
        cos_part = combine(
            [(math.cos(TWO_PI * (s * a % n) / n), even[s]) for s in range(n // 2 + 1)]
        )
        sin_part = combine([(math.sin(TWO_PI * (s * a % n) / n), odd[s]) for s in range(1, n // 2)])
        if sin_part is None:
            sin_part = jnp.zeros_like(cos_part)
        out.append((cos_part, sin_part))
    for a in range(n // 2 + 1, n):
        out.append((out[n - a][0], -out[n - a][1]))
    return out


def fused_kernel(
    shape,
    tokens_hbm,
    gain_hbm,
    w_in_hbm,
    chan_hbm,
    mid_hbm,
    pick_hbm,
    out_ref,
    tokens,
    gain,
    w_in,
    chan,
    mid,
    pick,
    natural,
    first_out,
    first_in,
    blocks,
    second_out,
    second_in,
    load_sem,
    send_a,
    recv_a,
    send_b,
    recv_b,
):
    row_count, col_count = shape
    peers = row_count * col_count
    tok_count, width = tokens.shape
    feat_count = w_in.shape[1]
    slots = feat_count // peers
    half = slots // 2
    per_lane = LANES // slots
    stacks = peers // per_lane
    fine = tok_count // peers
    members = GROUP_CH // slots
    groups = feat_count // GROUP_CH
    me = lax.axis_index("row") * col_count + lax.axis_index("col")

    def peer(step):
        return lax.rem(me + step, peers)

    def device(index):
        return {"row": index // col_count, "col": lax.rem(index, col_count)}

    row, col = lax.axis_index("row"), lax.axis_index("col")
    far_first = []
    for i in range(row_count - 1):
        down = row_count - 1 - i
        down = down - jnp.where(down <= row, 1, 0)
        up = i + jnp.where(i >= row, 1, 0)
        target_row = jnp.where(row * 2 < row_count, down, up)
        far_first += [
            target_row * col_count + lax.rem(col + shift, col_count)
            for shift in [*range(1, col_count), 0]
        ]
    far_first += [row * col_count + lax.rem(col + shift, col_count) for shift in range(1, col_count)]

    chunks = 4
    depth = width // chunks
    loads = [
        pltpu.make_async_copy(tokens_hbm, tokens, load_sem.at[0]),
        pltpu.make_async_copy(gain_hbm, gain, load_sem.at[1]),
    ]
    for i in range(chunks):
        part = pl.ds(i * depth, depth)
        loads.append(pltpu.make_async_copy(w_in_hbm.at[part], w_in.at[part], load_sem.at[2 + i]))
    rest = [(chan_hbm, chan), (mid_hbm, mid), (pick_hbm, pick)]
    for i, (src, dst) in enumerate(rest):
        loads.append(pltpu.make_async_copy(src, dst, load_sem.at[2 + chunks + i]))
    for load in loads[: 3 + chunks]:
        load.start()

    barrier = pltpu.get_barrier_semaphore()
    for step in range(1, peers):
        pl.semaphore_signal(barrier, inc=1, device_id=device(peer(step)), device_id_type=MESH)

    loads[0].wait()
    loads[1].wait()
    widened = tokens[...].astype(jnp.float32)
    factor = lax.rsqrt(jnp.mean(widened * widened, -1, keepdims=True) + NORM_EPS)
    normed = (widened * factor * gain[...].astype(jnp.float32).reshape(1, width)).astype(jnp.bfloat16)
    mixin = None
    for i in range(chunks):
        loads[2 + i].wait()
        term = jnp.dot(
            normed[:, i * depth : (i + 1) * depth],
            w_in[i * depth : (i + 1) * depth, :],
            preferred_element_type=jnp.float32,
        )
        mixin = term if mixin is None else mixin + term
    mixin = mixin.astype(jnp.bfloat16)
    for load in loads[3 + chunks :]:
        load.start()
    loads[2 + chunks].wait()
    for g in range(groups):
        spec = lax.dot_general(
            chan[...],
            mixin[:, g * GROUP_CH : (g + 1) * GROUP_CH],
            NT,
            preferred_element_type=jnp.float32,
        ).astype(jnp.bfloat16)
        for dd in range(members):
            first_out[g * members + dd] = spec[dd * slots : (dd + 1) * slots]
    pl.semaphore_wait(barrier, peers - 1)
    copies = []
    for step, target in enumerate(far_first):
        copy = pltpu.make_async_remote_copy(
            src_ref=first_out.at[target],
            dst_ref=first_in.at[me],
            send_sem=send_a.at[step],
            recv_sem=recv_a.at[me],
            device_id=device(target),
            device_id_type=MESH,
        )
        copy.start()
        copies.append(copy)
    first_in[me] = first_out[me]
    blocks[...] = jnp.zeros_like(blocks)
    for load in loads[3 + chunks :]:
        load.wait()
    for step in range(1, peers):
        source = peer(step)
        pltpu.make_async_copy(first_in.at[source], first_in.at[source], recv_a.at[source]).wait()

    arrived = [first_in[s].astype(jnp.float32) for s in range(peers)]
    place = lax.broadcasted_iota(jnp.int32, (half, tok_count), 0) + me * half
    paired = lax.rem(place, GROUP_CH // 2) != 0
    spectra = short_transform(arrived)
    for a, (cos_part, sin_part) in enumerate(spectra):
        a_cos, b_cos = cos_part[:half], cos_part[half:]
        a_sin, b_sin = sin_part[:half], sin_part[half:]
        top_cos = jnp.where(paired, a_cos + b_sin, a_cos)
        top_sin = jnp.where(paired, b_cos - a_sin, -a_sin)
        low_cos = jnp.where(paired, a_cos - b_sin, b_cos)
        low_sin = jnp.where(paired, -a_sin - b_cos, -b_sin)
        at = a % per_lane
        left = at * 2 * tok_count
        blocks[a // per_lane, at * slots : at * slots + half, left : left + tok_count] = (
            top_cos.astype(jnp.bfloat16)
        )
        blocks[
            a // per_lane, at * slots : at * slots + half, left + tok_count : left + 2 * tok_count
        ] = top_sin.astype(jnp.bfloat16)
        blocks[a // per_lane, at * slots + half : (at + 1) * slots, left : left + tok_count] = (
            low_cos.astype(jnp.bfloat16)
        )
        blocks[
            a // per_lane,
            at * slots + half : (at + 1) * slots,
            left + tok_count : left + 2 * tok_count,
        ] = low_sin.astype(jnp.bfloat16)
    found = []
    for g in range(stacks):
        value = lax.dot_general(mid[g], blocks[g], NT, preferred_element_type=jnp.float32)
        found.append(value.reshape(peers, fine, LANES))
    second_out[...] = jnp.concatenate(found, axis=1).astype(jnp.bfloat16)

    def landing(index):
        lanes = pl.ds(pl.multiple_of(lax.rem(index, members) * LANES, LANES), LANES)
        return second_in.at[index // members, :, lanes]

    returns = []
    for step, target in enumerate(far_first):
        copy = pltpu.make_async_remote_copy(
            src_ref=second_out.at[target],
            dst_ref=landing(me),
            send_sem=send_b.at[step],
            recv_sem=recv_b.at[me],
            device_id=device(target),
            device_id_type=MESH,
        )
        copy.start()
        returns.append(copy)
    landing(me)[...] = second_out[me]
    for copy in copies:
        copy.wait_send()
    for step in range(1, peers):
        source = peer(step)
        pltpu.make_async_copy(landing(source), landing(source), recv_b.at[source]).wait()
    flat = second_in[...].reshape(groups * stacks * fine, members * LANES)
    picked = jnp.dot(flat, pick[...], preferred_element_type=jnp.float32)
    for group in range(groups):
        for g in range(stacks):
            top = (group * stacks + g) * fine
            for a in range(per_lane):
                natural[group, pl.ds(g * per_lane + a, fine, stride=peers), :] = picked[top : top + fine, a * GROUP_CH : (a + 1) * GROUP_CH]
        out_ref[:, group * GROUP_CH : (group + 1) * GROUP_CH] = natural[group].astype(
            out_ref.dtype
        )
    for copy in returns:
        copy.wait_send()


def project_kernel(chunks, spectrum, w_out, out_hbm, staged, sems):
    size = w_out.shape[1] // chunks
    copies = []
    for i in range(chunks):
        lanes = slice(i * size, (i + 1) * size)
        staged[:, lanes] = jnp.dot(
            spectrum[...], w_out[:, lanes], preferred_element_type=jnp.float32
        ).astype(staged.dtype)
        span = pl.ds(i * size, size)
        copy = pltpu.make_async_copy(staged.at[:, span], out_hbm.at[:, span], sems.at[i])
        copy.start()
        copies.append(copy)
    for copy in copies:
        copy.wait()


def fused_shards(tokens, norm_gain, w_in, w_out):
    seq_count, tok_count, width = tokens.shape
    feat_count = w_in.shape[1]
    shape = (lax.axis_size("row"), lax.axis_size("col"))
    peers = shape[0] * shape[1]
    slots = feat_count // peers
    per_lane = LANES // slots
    stacks = peers // per_lane
    fine = tok_count // peers
    members = GROUP_CH // slots
    tables = host_tables(peers, tok_count, feat_count)
    operands = [tokens.reshape(tok_count, width), norm_gain, w_in, *tables]
    held = [pltpu.VMEM(x.shape, x.dtype) for x in operands]
    spectrum = pl.pallas_call(
        functools.partial(fused_kernel, shape),
        out_shape=pltpu.VMEM((tok_count, feat_count), jnp.bfloat16),
        in_specs=[pl.BlockSpec(memory_space=pltpu.HBM)] * len(operands),
        out_specs=pl.BlockSpec(memory_space=pltpu.VMEM),
        scratch_shapes=held
        + [
            pltpu.VMEM((feat_count // GROUP_CH, tok_count, GROUP_CH), jnp.float32),
            pltpu.VMEM((peers, slots, tok_count), jnp.bfloat16),
            pltpu.VMEM((peers, slots, tok_count), jnp.bfloat16),
            pltpu.VMEM((stacks, LANES, per_lane * 2 * tok_count), jnp.bfloat16),
            pltpu.VMEM((peers, stacks * fine, LANES), jnp.bfloat16),
            pltpu.VMEM((peers // members, stacks * fine, members * LANES), jnp.bfloat16),
            pltpu.SemaphoreType.DMA((16,)),
            pltpu.SemaphoreType.DMA((peers,)),
            pltpu.SemaphoreType.DMA((peers,)),
            pltpu.SemaphoreType.DMA((peers,)),
            pltpu.SemaphoreType.DMA((peers,)),
        ],
        compiler_params=pltpu.CompilerParams(
            collective_id=0, has_side_effects=True, vmem_limit_bytes=64_600_000
        ),
    )(*operands)
    chunks = max(1, width // 512)
    mixed = pl.pallas_call(
        functools.partial(project_kernel, chunks),
        out_shape=jax.ShapeDtypeStruct((tok_count, width), jnp.bfloat16),
        in_specs=[pl.BlockSpec(memory_space=pltpu.VMEM)] * 2,
        out_specs=pl.BlockSpec(memory_space=pltpu.HBM),
        scratch_shapes=[
            pltpu.VMEM((tok_count, width), jnp.bfloat16),
            pltpu.SemaphoreType.DMA((chunks,)),
        ],
        compiler_params=pltpu.CompilerParams(vmem_limit_bytes=8 * 1024 * 1024),
    )(spectrum, w_out)
    return mixed.reshape(seq_count, tok_count, width)


def shards(tokens, norm_gain, w_in, w_out):
    peers = lax.axis_size("row") * lax.axis_size("col")
    seq_count, tok_count, _ = tokens.shape
    if seq_count == 1 and fused_fits(peers, tok_count, w_in.shape[1]):
        return fused_shards(tokens, norm_gain, w_in, w_out)
    return factored_shards(tokens, norm_gain, w_in, w_out)


def solution(mesh):
    return jax.shard_map(
        shards,
        mesh=mesh,
        in_specs=(P("grp", ("row", "col"), None), P(), P(), P()),
        out_specs=P("grp", ("row", "col"), None),
        check_vma=False,
    )
```
